32 devices in a mesh: rep: 2 (over x), fs: 8 (over z, y), tp: 2 (over core).
Axes of the slice: x: 2, y: 2, z: 4, core: 2. Of those that a mesh axis runs over, the one named last changes fastest.
Arguments:
- tokens: bfloat16 [16, 1024, 2048], P(('rep', 'fs'), 'tp'), may hold values from -6 to 6
- mix_gain: float32 [2048], replicated, may hold values from 0.1 to 1.9
- out_gate_w: float32 [2048, 1024], P('fs', 'tp'), may hold values from -0.125 to 0.125
- in_gate_w: float32 [2048, 1024], P('fs', 'tp'), may hold values from -0.125 to 0.125
- value_w: float32 [2048, 1024], P('fs', 'tp'), may hold values from -0.125 to 0.125
- out_gate_scale: float32 [1024], P(('tp', 'fs')), may hold values from 0.28 to 3.5
- in_gate_scale: float32 [1024], P(('tp', 'fs')), may hold values from 0.5 to 2
- value_scale: float32 [1024], P(('tp', 'fs')), may hold values from 0.5 to 2
- mix_taps: float32 [3, 1024], P(None, 'tp'), may hold values from -3.5 to 3.5
- conv_gain: float32 [1024], P('tp'), may hold values from 0.1 to 1.9
- out_proj_w: float32 [1024, 2048], P('tp', 'fs'), may hold values from -0.1875 to 0.1875
- proj_scale: float32 [2048], P('fs'), may hold values from 0.5 to 2
- ffn_gain: float32 [2048], replicated, may hold values from 0.1 to 1.9
- gate_w: float32 [2048, 2816], P('fs', 'tp'), may hold values from -0.125 to 0.125
- up_w: float32 [2048, 2816], P('fs', 'tp'), may hold values from -0.125 to 0.125
- gate_scale: float32 [2816], P(('tp', 'fs')), may hold values from 0.5 to 2
- up_scale: float32 [2816], P(('tp', 'fs')), may hold values from 0.5 to 2
- gate_taps: float32 [3, 2816], P(None, 'tp'), may hold values from -3.5 to 3.5
- up_taps: float32 [3, 2816], P(None, 'tp'), may hold values from -3.5 to 3.5
- gate_bias: float32 [2816], P('tp'), may hold values from -3 to 3
- up_bias: float32 [2816], P('tp'), may hold values from -3 to 3
- down_w: float32 [2816, 2048], P('tp', 'fs'), may hold values from -0.109375 to 0.109375
- down_scale: float32 [2048], P('fs'), may hold values from 0.5 to 2
Outputs:
- layer_out: bfloat16 [16, 1024, 2048], P(('rep', 'fs'), 'tp')
The draws below stay inside these ranges and needn't reach their ends.
All inputs are finite; a program needn't handle non-finite values.
Results may differ from the reference program's by a relative error of at most 0.02.
Values may be sent and summed in bfloat16 or wider, within the bound.
A program may use at most 128 MiB of HBM per device.

```python
import math
import jax
import jax.numpy as jnp
from jax import lax

D = 2048
CONV = 1024
FF = 2816
KW = 3
SEQ = 1024
SEQS = 16


def draw_out_gate_scale(key, part):
    ramp = jnp.exp(jnp.linspace(math.log(0.4), math.log(2.5), CONV)).astype(jnp.float32)
    noise = jax.random.uniform(key, (CONV,), jnp.float32, 0.7, 1.4)
    return ramp * noise


def block_scale(rng, dims, pieces, low, top_value):
    loudness, own = 1.0, jax.random.fold_in(rng, 6)
    for dim, blocks in pieces:
        steps = jnp.exp(jax.random.uniform(jax.random.fold_in(own, dim), (blocks,), jnp.float32, low / len(pieces), top_value / len(pieces)))
        loudness = loudness * jnp.repeat(steps, dims[dim] // blocks).reshape([-1 if axis == dim else 1 for axis in range(len(dims))])
    return loudness


def bell_draw(key, extent, width, limit, cuts=(), held_as=jnp.bfloat16):
    result = jax.random.normal(key, extent, jnp.float32) * width
    if len(cuts) > 0:
        result = block_scale(key, extent, cuts, -0.22, 0.18) * result
    return jnp.clip(result, min=-limit, max=limit).astype(held_as)


def setup_inputs(seed: int = 0) -> dict:
    streams_of = jax.random.split(jax.random.key(seed), 24)
    tokens = bell_draw(streams_of[0], (SEQS, SEQ, D), 1.0, 6.0, ((0, 16), (1, 2)))
    mix_gain = jnp.clip(1.0 + 0.18 * jax.random.normal(streams_of[1], (D,), jnp.float32), 0.1, 1.9)
    out_gate_w = bell_draw(streams_of[2], (D, CONV), D ** -0.5, 0.125, ((0, 8), (1, 2)), jnp.float32)
    in_gate_w = bell_draw(streams_of[3], (D, CONV), D ** -0.5, 0.125, ((0, 8), (1, 2)), jnp.float32)
    value_w = bell_draw(streams_of[4], (D, CONV), D ** -0.5, 0.125, ((0, 8), (1, 2)), jnp.float32)
    out_gate_scale = draw_out_gate_scale(jax.random.fold_in(streams_of[23], 71), 0)
    in_gate_scale = jnp.clip(jnp.exp(math.log(2.0) - 1.3862944 * jax.random.uniform(streams_of[6], (CONV,), jnp.float32) ** block_scale(streams_of[6], (CONV,), ((0, 16),), -0.2, 0.2)), 0.5, 2.0)
    value_scale = jnp.clip(jnp.exp(math.log(2.0) - 1.3862944 * jax.random.uniform(streams_of[7], (CONV,), jnp.float32) ** block_scale(streams_of[7], (CONV,), ((0, 16),), -0.2, 0.2)), 0.5, 2.0)
    mix_taps = bell_draw(streams_of[8], (KW, CONV), KW ** -0.5, 3.5, ((1, 2),), jnp.float32)
    conv_gain = jnp.clip(1.0 + 0.18 * jax.random.normal(streams_of[9], (CONV,), jnp.float32), 0.1, 1.9)
    out_proj_w = bell_draw(streams_of[10], (CONV, D), CONV ** -0.5, 0.1875, ((0, 2), (1, 8)), jnp.float32)
    proj_scale = jnp.clip(jnp.exp(math.log(2.0) - 1.3862944 * jax.random.uniform(streams_of[11], (D,), jnp.float32) ** block_scale(streams_of[11], (D,), ((0, 8),), -0.2, 0.2)), 0.5, 2.0)
    ffn_gain = jnp.clip(1.0 + 0.18 * jax.random.normal(streams_of[12], (D,), jnp.float32), 0.1, 1.9)
    gate_w = bell_draw(streams_of[13], (D, FF), D ** -0.5, 0.125, ((0, 8), (1, 2)), jnp.float32)
    up_w = bell_draw(streams_of[14], (D, FF), D ** -0.5, 0.125, ((0, 8), (1, 2)), jnp.float32)
    gate_scale = jnp.clip(jnp.exp(math.log(2.0) - 1.3862944 * jax.random.uniform(streams_of[15], (FF,), jnp.float32) ** block_scale(streams_of[15], (FF,), ((0, 16),), -0.2, 0.2)), 0.5, 2.0)
    up_scale = jnp.clip(jnp.exp(math.log(2.0) - 1.3862944 * jax.random.uniform(streams_of[16], (FF,), jnp.float32) ** block_scale(streams_of[16], (FF,), ((0, 16),), -0.2, 0.2)), 0.5, 2.0)
    gate_taps = bell_draw(streams_of[17], (KW, FF), KW ** -0.5, 3.5, ((1, 2),), jnp.float32)
    up_taps = bell_draw(streams_of[18], (KW, FF), KW ** -0.5, 3.5, ((1, 2),), jnp.float32)
    gate_bias = bell_draw(streams_of[19], (FF,), 0.5, 3.0, ((0, 2),), jnp.float32)
    up_bias = bell_draw(streams_of[20], (FF,), 0.5, 3.0, ((0, 2),), jnp.float32)
    down_w = bell_draw(streams_of[21], (FF, D), FF ** -0.5, 0.109375, ((0, 2), (1, 8)), jnp.float32)
    down_scale = jnp.clip(jnp.exp(math.log(2.0) - 1.3862944 * jax.random.uniform(streams_of[22], (D,), jnp.float32) ** block_scale(streams_of[22], (D,), ((0, 8),), -0.2, 0.2)), 0.5, 2.0)
    return {"tokens": tokens, "mix_gain": mix_gain, "out_gate_w": out_gate_w, "in_gate_w": in_gate_w, "value_w": value_w, "out_gate_scale": out_gate_scale, "in_gate_scale": in_gate_scale, "value_scale": value_scale, "mix_taps": mix_taps, "conv_gain": conv_gain, "out_proj_w": out_proj_w, "proj_scale": proj_scale, "ffn_gain": ffn_gain, "gate_w": gate_w, "up_w": up_w, "gate_scale": gate_scale, "up_scale": up_scale, "gate_taps": gate_taps, "up_taps": up_taps, "gate_bias": gate_bias, "up_bias": up_bias, "down_w": down_w, "down_scale": down_scale}


epsilon = 1e-06

def norm_rows(values, gain):
    return values * lax.rsqrt(lax.optimization_barrier(jnp.mean(values * values, axis=-1, keepdims=True)) + epsilon) * gain

def causal_taps(values, taps):
    kernel = taps.shape[0]
    length = values.shape[0]
    padded = jnp.pad(values, ((kernel - 1, 0), (0, 0)))
    total = jnp.zeros(values.shape, jnp.float32)
    for offset in range(kernel):
        total = total + taps[offset] * padded[offset:offset + length]
    return total

def reference(tokens, mix_gain, out_gate_w, in_gate_w, value_w, out_gate_scale, in_gate_scale, value_scale, mix_taps, conv_gain, out_proj_w, proj_scale, ffn_gain, gate_w, up_w, gate_scale, up_scale, gate_taps, up_taps, gate_bias, up_bias, down_w, down_scale):

    def project(left, weight, scale):
        return jnp.dot(left, weight.astype(jnp.bfloat16), preferred_element_type=jnp.float32) * scale

    def layer_one(sequence):
        resid = sequence.astype(jnp.float32)
        normed_in = norm_rows(resid, mix_gain).astype(jnp.bfloat16)
        out_gate = project(normed_in, out_gate_w, out_gate_scale).astype(jnp.bfloat16)
        in_gate = project(normed_in, in_gate_w, in_gate_scale).astype(jnp.bfloat16)
        value_in = project(normed_in, value_w, value_scale).astype(jnp.bfloat16)
        mixed_in = in_gate.astype(jnp.float32) * value_in.astype(jnp.float32)
        conv_out = (out_gate.astype(jnp.float32) * causal_taps(mixed_in, mix_taps)).astype(jnp.bfloat16)
        mixed = norm_rows(conv_out.astype(jnp.float32), conv_gain).astype(jnp.bfloat16)
        first = (resid + project(mixed, out_proj_w, proj_scale)).astype(jnp.bfloat16)
        resid_two = first.astype(jnp.float32)
        normed_ffn = norm_rows(resid_two, ffn_gain).astype(jnp.bfloat16)
        gate_pre = project(normed_ffn, gate_w, gate_scale).astype(jnp.bfloat16)
        up_pre = project(normed_ffn, up_w, up_scale).astype(jnp.bfloat16)
        gate_act = causal_taps(gate_pre.astype(jnp.float32), gate_taps) + gate_bias
        up_act = causal_taps(up_pre.astype(jnp.float32), up_taps) + up_bias
        hidden = (jax.nn.silu(gate_act) * up_act).astype(jnp.bfloat16)
        return (resid_two + project(hidden, down_w, down_scale)).astype(jnp.bfloat16)
    return lax.map(layer_one, tokens)
```

```python
import functools

import jax
import jax.numpy as jnp
from jax import lax
from jax.experimental import pallas as pl
from jax.experimental.pallas import tpu as pltpu
from jax.sharding import PartitionSpec as P

MESH = pl.DeviceIdType.MESH
epsilon = 1e-06


def split_rows(rows, step):
    a = max((rows * 3 // 8) // step, 1) * step
    return a, rows - 2 * a


class Gather:
    def __init__(self, sizes, srcs, dsts, steps, sems):
        self.srcs, self.dsts, self.steps = srcs, dsts, steps
        self.fs = sizes["fs"]
        self.ny = 2
        self.nz = self.fs // self.ny
        self.me = lax.axis_index("fs")
        self.x = lax.axis_index("rep")
        self.y = self.me % self.ny
        self.z = self.me // self.ny
        self.sz, self.rz, self.sy, self.ry, self.sx, self.rx = sems
        self.left = {"fs": self.me - self.ny}
        self.right = {"fs": self.me + self.ny}
        self.across = {"fs": self.z * self.ny + 1 - self.y}
        self.other = {"rep": 1 - self.x}

    def barrier(self):
        sem = pltpu.get_barrier_semaphore()
        has_left = self.z > 0
        has_right = self.z < self.nz - 1

        @pl.when(has_left)
        def _():
            pl.semaphore_signal(sem, inc=1, device_id=self.left, device_id_type=MESH)

        @pl.when(has_right)
        def _():
            pl.semaphore_signal(sem, inc=1, device_id=self.right, device_id_type=MESH)

        pl.semaphore_signal(sem, inc=1, device_id=self.across, device_id_type=MESH)
        pl.semaphore_signal(sem, inc=1, device_id=self.other, device_id_type=MESH)
        pl.semaphore_wait(sem, 2 + has_left.astype(jnp.int32) + has_right.astype(jnp.int32))

    def part(self, c, x, short):
        rows = self.srcs[c].shape[0]
        a, b = split_rows(rows, self.steps[c])
        if short:
            return pl.ds(pl.multiple_of(x * (a + b), self.steps[c]), a)
        return pl.ds(pl.multiple_of(x * a, self.steps[c]), a + b)

    def copy(self, c, origin, rows, send, recv, target, own=False):
        dst = self.dsts[c].at[origin, rows]
        return pltpu.make_async_remote_copy(
            src_ref=self.srcs[c].at[rows] if own else dst,
            dst_ref=dst,
            send_sem=send,
            recv_sem=recv,
            device_id=target,
            device_id_type=MESH,
        )

    def along(self, c, way, hop, own=False):
        origin = self.me - (hop - 1) * self.ny if way == 0 else self.me + (hop - 1) * self.ny
        target = self.right if way == 0 else self.left
        return self.copy(
            c, origin, self.part(c, self.x, False), self.sz.at[c, way, hop], self.rz.at[c, way, hop], target, own
        )

    def sends(self, way, hop):
        if way == 0:
            return (self.z < self.nz - 1) & (self.z - (hop - 1) >= 0)
        return (self.z > 0) & (self.z + (hop - 1) <= self.nz - 1)

    def arrives(self, way, hop):
        return self.z - hop >= 0 if way == 0 else self.z + hop <= self.nz - 1

    def over_y(self, c, slot, origin, own=False):
        return self.copy(
            c, origin, self.part(c, self.x, False), self.sy.at[c, slot], self.ry.at[c, slot], self.across, own
        )

    def over_x(self, c, slot, origin):
        return self.copy(c, origin, self.part(c, self.x, True), self.sx.at[c, slot], self.rx.at[c, slot], self.other)

    def origin(self, way, hop):
        return self.me - hop * self.ny if way == 0 else self.me + hop * self.ny

    def mirror(self, origin):
        return origin + 1 - 2 * self.y

    def start_own(self, c):
        for way in range(2):
            pl.when(self.sends(way, 1))(lambda way=way: self.along(c, way, 1, True).start())
        self.over_y(c, 0, self.me, True).start()

    def z_arrival(self, c, hop):
        for way in range(2):
            slot = 2 * hop - 1 + way
            origin = self.origin(way, hop)

            @pl.when(self.arrives(way, hop))
            def _():
                self.along(c, way, hop).wait_recv()
                if hop < self.nz - 1:
                    pl.when(self.sends(way, hop + 1))(lambda: self.along(c, way, hop + 1).start())
                self.over_y(c, slot, origin).start()
                self.over_x(c, slot, origin).start()

    def y_arrival(self, c, hop):
        for way in range(2 if hop else 1):
            slot = 2 * hop - 1 + way if hop else 0
            origin = self.mirror(self.origin(way, hop))

            def go():
                self.over_y(c, slot, origin).wait_recv()
                self.over_x(c, 2 * self.nz + slot, origin).start()

            pl.when(self.arrives(way, hop))(go) if hop else go()

    def x_arrivals(self, c):
        for hop in range(self.nz):
            for way in range(2 if hop else 1):
                slot = 2 * hop - 1 + way if hop else 0
                near = self.origin(way, hop)

                def go():
                    for base, origin in ((0, near), (2 * self.nz, self.mirror(near))):
                        if base or hop:
                            rows = self.part(c, 1 - self.x, True)
                            self.copy(
                                c, origin, rows, self.sx.at[c, base + slot], self.rx.at[c, base + slot], self.other
                            ).wait_recv()

                pl.when(self.arrives(way, hop))(go) if hop else go()

    def finish(self, c):
        for hop in range(self.nz):
            for way in range(2):
                if hop + 1 < self.nz:
                    pl.when(self.sends(way, hop + 1))(
                        lambda way=way, hop=hop: self.along(c, way, hop + 1).wait_send()
                    )
                if hop == 0 and way == 1:
                    continue
                slot = 2 * hop - 1 + way if hop else 0
                near = self.origin(way, hop)

                def go():
                    self.over_y(c, slot, near).wait_send()
                    self.over_x(c, 2 * self.nz + slot, self.mirror(near)).wait_send()
                    if hop:
                        self.over_x(c, slot, near).wait_send()

                pl.when(self.arrives(way, hop))(go) if hop else go()


def gather_kernel(sizes, steps, count, *refs):
    srcs, dsts = refs[:count], refs[count : 2 * count]
    sems, own_sem = refs[2 * count : -1], refs[-1]
    g = Gather(sizes, srcs, dsts, steps, sems)
    own = [pltpu.make_async_copy(srcs[c], dsts[c].at[g.me], own_sem.at[c]) for c in range(count)]
    g.barrier()
    g.start_own(0)
    for copy in own:
        copy.start()
    for c in range(count + 1):
        if c + 1 < count:
            g.start_own(c + 1)
        for hop in range(g.nz):
            if hop and c < count:
                g.z_arrival(c, hop)
            if c:
                g.y_arrival(c - 1, hop)
    for c in range(count):
        g.x_arrivals(c)
        g.finish(c)
        own[c].wait()


def gather_all(sizes, srcs, steps):
    fs = sizes["fs"]
    nz, count = fs // 2, len(srcs)
    dma = pltpu.SemaphoreType.DMA
    return pl.pallas_call(
        functools.partial(gather_kernel, sizes, steps, count),
        out_shape=[jax.ShapeDtypeStruct((fs,) + s.shape, s.dtype) for s in srcs],
        in_specs=[pl.BlockSpec(memory_space=pl.ANY)] * count,
        out_specs=[pl.BlockSpec(memory_space=pl.ANY)] * count,
        scratch_shapes=[
            dma((count, 2, nz)),
            dma((count, 2, nz)),
            dma((count, 2 * nz)),
            dma((count, 2 * nz)),
            dma((count, 4 * nz)),
            dma((count, 4 * nz)),
            dma((count,)),
        ],
        compiler_params=pltpu.CompilerParams(collective_id=0, has_side_effects=True),
    )(*srcs)


def norm_rows(values, gain):
    return values * lax.rsqrt(jnp.mean(values * values, axis=-1, keepdims=True) + epsilon) * gain


def causal_taps(values, taps):
    kernel = taps.shape[0]
    length = values.shape[0]
    padded = jnp.pad(values, ((kernel - 1, 0), (0, 0)))
    total = jnp.zeros(values.shape, jnp.float32)
    for offset in range(kernel):
        total = total + taps[offset] * padded[offset : offset + length]
    return total


def column_block(left, scale_all, piece):
    return jnp.dot(left, piece, preferred_element_type=jnp.float32) * scale_all


def local(
    sizes,
    tokens,
    mix_gain,
    out_gate_w,
    in_gate_w,
    value_w,
    out_gate_scale,
    in_gate_scale,
    value_scale,
    mix_taps,
    conv_gain,
    out_proj_w,
    proj_scale,
    ffn_gain,
    gate_w,
    up_w,
    gate_scale,
    up_scale,
    gate_taps,
    up_taps,
    gate_bias,
    up_bias,
    down_w,
    down_scale,
):
    resid = tokens[0].astype(jnp.float32)
    normed_in = norm_rows(resid, mix_gain).astype(jnp.bfloat16)
    all_rows = lax.all_gather(normed_in, "tp", axis=0, tiled=True)
    vectors = [out_gate_scale, in_gate_scale, value_scale, gate_scale, up_scale, proj_scale, down_scale]
    flat = jnp.concatenate(vectors)
    lines = 24 * (-(-flat.shape[0] // (24 * 128)))
    flat = jnp.pad(flat, (0, lines * 128 - flat.shape[0])).reshape(lines, 128)
    half = jnp.bfloat16
    mix_w = jnp.concatenate([out_gate_w.astype(half), in_gate_w.astype(half), value_w.astype(half)], axis=1)
    flats, mix_all, proj_all, gate_all, up_all, down_all = gather_all(
        sizes,
        [flat, mix_w, out_proj_w.astype(half), gate_w.astype(half), up_w.astype(half), down_w.astype(half)],
        [8, 16, 16, 16, 16, 16],
    )
    fs = sizes["fs"]
    flats = flats.reshape(fs, -1)
    scales, at = [], 0
    for vector in vectors:
        scales.append(flats[:, at : at + vector.shape[0]].reshape(-1))
        at += vector.shape[0]
    whole_outgate, whole_ingate, whole_value, whole_gate, whole_up, whole_proj, whole_down = scales
    mix_full = mix_all.reshape(-1, mix_w.shape[1])
    width = out_gate_w.shape[1]
    outgate_rows, ingate_rows, value_rows = (
        mix_full[:, :width],
        mix_full[:, width : 2 * width],
        mix_full[:, 2 * width :],
    )
    proj_cols = proj_all.transpose(1, 0, 2).reshape(proj_all.shape[1], -1)
    down_cols = down_all.transpose(1, 0, 2).reshape(down_all.shape[1], -1)
    out_gate = (
        jnp.dot(all_rows, outgate_rows, preferred_element_type=jnp.float32) * whole_outgate
    ).astype(jnp.bfloat16)
    in_gate = (
        jnp.dot(all_rows, ingate_rows, preferred_element_type=jnp.float32) * whole_ingate
    ).astype(jnp.bfloat16)
    value_in = (
        jnp.dot(all_rows, value_rows, preferred_element_type=jnp.float32) * whole_value
    ).astype(jnp.bfloat16)
    mixed_in = in_gate.astype(jnp.float32) * value_in.astype(jnp.float32)
    conv_out = (out_gate.astype(jnp.float32) * causal_taps(mixed_in, mix_taps)).astype(jnp.bfloat16)
    conv_float = conv_out.astype(jnp.float32)
    channels = conv_float.shape[1] * lax.axis_size("tp")
    sumsq = lax.psum(jnp.sum(conv_float * conv_float, axis=1), "tp")
    mixed = (conv_float * lax.rsqrt(sumsq / channels + epsilon)[:, None] * conv_gain).astype(
        jnp.bfloat16
    )
    partial_mix = column_block(
        mixed, whole_proj, proj_cols
    )
    summed = lax.psum_scatter(
        partial_mix.astype(jnp.bfloat16), "tp", scatter_dimension=0, tiled=True
    ).astype(jnp.float32)
    first = (resid + summed).astype(jnp.bfloat16)
    resid_two = first.astype(jnp.float32)
    normed_ffn = norm_rows(resid_two, ffn_gain).astype(jnp.bfloat16)
    ffn_all = lax.all_gather(normed_ffn, "tp", axis=0, tiled=True)
    gate_full = gate_all.reshape(-1, gate_w.shape[1])
    up_full = up_all.reshape(-1, up_w.shape[1])
    gate_sum = jnp.dot(ffn_all, gate_full, preferred_element_type=jnp.float32)
    up_sum = jnp.dot(ffn_all, up_full, preferred_element_type=jnp.float32)
    gate_pre = (gate_sum * whole_gate).astype(jnp.bfloat16)
    up_pre = (up_sum * whole_up).astype(jnp.bfloat16)
    gate_act = causal_taps(gate_pre.astype(jnp.float32), gate_taps) + gate_bias
    up_act = causal_taps(up_pre.astype(jnp.float32), up_taps) + up_bias
    hidden = (jax.nn.silu(gate_act) * up_act).astype(jnp.bfloat16)
    partial_down = column_block(
        hidden, whole_down, down_cols
    )
    summed_two = lax.psum_scatter(
        partial_down.astype(jnp.bfloat16), "tp", scatter_dimension=0, tiled=True
    ).astype(jnp.float32)
    return (resid_two + summed_two).astype(jnp.bfloat16)[None]


def solution(mesh):
    placed = (
        P(("rep", "fs"), "tp", None),
        P(),
        P("fs", "tp"),
        P("fs", "tp"),
        P("fs", "tp"),
        P(("tp", "fs")),
        P(("tp", "fs")),
        P(("tp", "fs")),
        P(None, "tp"),
        P("tp"),
        P("tp", "fs"),
        P("fs"),
        P(),
        P("fs", "tp"),
        P("fs", "tp"),
        P(("tp", "fs")),
        P(("tp", "fs")),
        P(None, "tp"),
        P(None, "tp"),
        P("tp"),
        P("tp"),
        P("tp", "fs"),
        P("fs"),
    )
    return jax.shard_map(
        functools.partial(local, dict(mesh.shape)), mesh=mesh, in_specs=placed, out_specs=P(("rep", "fs"), "tp", None), check_vma=False
    )
```

```python
import functools

import jax
import jax.numpy as jnp
from jax import lax
from jax.experimental import pallas as pl
from jax.experimental.pallas import tpu as pltpu
from jax.sharding import PartitionSpec as P

MESH = pl.DeviceIdType.MESH
epsilon = 1e-06


def split_rows(rows, step):
    a = max((rows * 3 // 8) // step, 1) * step
    return a, rows - 2 * a


class Gather:
    def __init__(self, sizes, srcs, dsts, steps, sems):
        self.srcs, self.dsts, self.steps = srcs, dsts, steps
        self.fs = sizes["fs"]
        self.ny = 2
        self.nz = self.fs // self.ny
        self.me = lax.axis_index("fs")
        self.x = lax.axis_index("rep")
        self.y = self.me % self.ny
        self.z = self.me // self.ny
        self.sz, self.rz, self.sy, self.ry, self.sx, self.rx = sems
        self.left = {"fs": self.me - self.ny}
        self.right = {"fs": self.me + self.ny}
        self.across = {"fs": self.z * self.ny + 1 - self.y}
        self.other = {"rep": 1 - self.x}

    def barrier(self):
        sem = pltpu.get_barrier_semaphore()
        has_left = self.z > 0
        has_right = self.z < self.nz - 1

        @pl.when(has_left)
        def _():
            pl.semaphore_signal(sem, inc=1, device_id=self.left, device_id_type=MESH)

        @pl.when(has_right)
        def _():
            pl.semaphore_signal(sem, inc=1, device_id=self.right, device_id_type=MESH)

        pl.semaphore_signal(sem, inc=1, device_id=self.across, device_id_type=MESH)
        pl.semaphore_signal(sem, inc=1, device_id=self.other, device_id_type=MESH)
        pl.semaphore_wait(sem, 2 + has_left.astype(jnp.int32) + has_right.astype(jnp.int32))

    def part(self, c, x, short):
        rows = self.srcs[c].shape[0]
        a, b = split_rows(rows, self.steps[c])
        if short:
            return pl.ds(pl.multiple_of(x * (a + b), self.steps[c]), a)
        return pl.ds(pl.multiple_of(x * a, self.steps[c]), a + b)

    def copy(self, c, origin, rows, send, recv, target, own=False):
        dst = self.dsts[c].at[origin, rows]
        return pltpu.make_async_remote_copy(
            src_ref=self.srcs[c].at[rows] if own else dst,
            dst_ref=dst,
            send_sem=send,
            recv_sem=recv,
            device_id=target,
            device_id_type=MESH,
        )

    def along(self, c, way, hop, own=False):
        origin = self.me - (hop - 1) * self.ny if way == 0 else self.me + (hop - 1) * self.ny
        target = self.right if way == 0 else self.left
        return self.copy(
            c, origin, self.part(c, self.x, False), self.sz.at[c, way, hop], self.rz.at[c, way, hop], target, own
        )

    def sends(self, way, hop):
        if way == 0:
            return (self.z < self.nz - 1) & (self.z - (hop - 1) >= 0)
        return (self.z > 0) & (self.z + (hop - 1) <= self.nz - 1)

    def arrives(self, way, hop):
        return self.z - hop >= 0 if way == 0 else self.z + hop <= self.nz - 1

    def over_y(self, c, slot, origin, own=False):
        return self.copy(
            c, origin, self.part(c, self.x, False), self.sy.at[c, slot], self.ry.at[c, slot], self.across, own
        )

    def over_x(self, c, slot, origin):
        return self.copy(c, origin, self.part(c, self.x, True), self.sx.at[c, slot], self.rx.at[c, slot], self.other)

    def origin(self, way, hop):
        return self.me - hop * self.ny if way == 0 else self.me + hop * self.ny

    def mirror(self, origin):
        return origin + 1 - 2 * self.y

    def start_own(self, c):
        for way in range(2):
            pl.when(self.sends(way, 1))(lambda way=way: self.along(c, way, 1, True).start())
        self.over_y(c, 0, self.me, True).start()

    def z_arrival(self, c, hop):
        for way in range(2):
            slot = 2 * hop - 1 + way
            origin = self.origin(way, hop)

            @pl.when(self.arrives(way, hop))
            def _():
                self.along(c, way, hop).wait_recv()
                if hop < self.nz - 1:
                    pl.when(self.sends(way, hop + 1))(lambda: self.along(c, way, hop + 1).start())
                self.over_y(c, slot, origin).start()
                self.over_x(c, slot, origin).start()

    def y_arrival(self, c, hop):
        for way in range(2 if hop else 1):
            slot = 2 * hop - 1 + way if hop else 0
            origin = self.mirror(self.origin(way, hop))

            def go():
                self.over_y(c, slot, origin).wait_recv()
                self.over_x(c, 2 * self.nz + slot, origin).start()

            pl.when(self.arrives(way, hop))(go) if hop else go()

    def x_arrivals(self, c):
        for hop in range(self.nz):
            for way in range(2 if hop else 1):
                slot = 2 * hop - 1 + way if hop else 0
                near = self.origin(way, hop)

                def go():
                    for base, origin in ((0, near), (2 * self.nz, self.mirror(near))):
                        if base or hop:
                            rows = self.part(c, 1 - self.x, True)
                            self.copy(
                                c, origin, rows, self.sx.at[c, base + slot], self.rx.at[c, base + slot], self.other
                            ).wait_recv()

                pl.when(self.arrives(way, hop))(go) if hop else go()

    def finish(self, c):
        for hop in range(self.nz):
            for way in range(2):
                if hop + 1 < self.nz:
                    pl.when(self.sends(way, hop + 1))(
                        lambda way=way, hop=hop: self.along(c, way, hop + 1).wait_send()
                    )
                if hop == 0 and way == 1:
                    continue
                slot = 2 * hop - 1 + way if hop else 0
                near = self.origin(way, hop)

                def go():
                    self.over_y(c, slot, near).wait_send()
                    self.over_x(c, 2 * self.nz + slot, self.mirror(near)).wait_send()
                    if hop:
                        self.over_x(c, slot, near).wait_send()

                pl.when(self.arrives(way, hop))(go) if hop else go()


def gather_kernel(sizes, steps, count, *refs):
    srcs, dsts = refs[:count], refs[count : 2 * count]
    sems, own_sem = refs[2 * count : -1], refs[-1]
    g = Gather(sizes, srcs, dsts, steps, sems)
    own = [pltpu.make_async_copy(srcs[c], dsts[c].at[g.me], own_sem.at[c]) for c in range(count)]
    g.barrier()
    g.start_own(0)
    for copy in own:
        copy.start()
    for c in range(count + 1):
        if c + 1 < count:
            g.start_own(c + 1)
        for hop in range(g.nz):
            if hop and c < count:
                g.z_arrival(c, hop)
            if c:
                g.y_arrival(c - 1, hop)
    for c in range(count):
        g.x_arrivals(c)
        g.finish(c)
        own[c].wait()


def gather_all(sizes, srcs, steps):
    fs = sizes["fs"]
    nz, count = fs // 2, len(srcs)
    dma = pltpu.SemaphoreType.DMA
    return pl.pallas_call(
        functools.partial(gather_kernel, sizes, steps, count),
        out_shape=[jax.ShapeDtypeStruct((fs,) + s.shape, s.dtype) for s in srcs],
        in_specs=[pl.BlockSpec(memory_space=pl.ANY)] * count,
        out_specs=[pl.BlockSpec(memory_space=pl.ANY)] * count,
        scratch_shapes=[
            dma((count, 2, nz)),
            dma((count, 2, nz)),
            dma((count, 2 * nz)),
            dma((count, 2 * nz)),
            dma((count, 4 * nz)),
            dma((count, 4 * nz)),
            dma((count,)),
        ],
        compiler_params=pltpu.CompilerParams(collective_id=0, has_side_effects=True),
    )(*srcs)


def norm_rows(values, gain):
    return values * lax.rsqrt(jnp.mean(values * values, axis=-1, keepdims=True) + epsilon) * gain


def causal_taps(values, taps):
    kernel = taps.shape[0]
    length = values.shape[0]
    padded = jnp.pad(values, ((kernel - 1, 0), (0, 0)))
    total = jnp.zeros(values.shape, jnp.float32)
    for offset in range(kernel):
        total = total + taps[offset] * padded[offset : offset + length]
    return total


def column_block(left, scale_all, piece):
    return jnp.dot(left, piece, preferred_element_type=jnp.float32) * scale_all


def summed_half(sizes, left, scale_all, piece):
    if sizes["tp"] != 2:
        partial = column_block(left, scale_all, piece).astype(jnp.bfloat16)
        return lax.psum_scatter(partial, "tp", scatter_dimension=0, tiled=True).astype(jnp.float32)
    here = lax.axis_index("tp")
    rows = left.shape[0] // 2
    theirs = lax.dynamic_slice_in_dim(left, (1 - here) * rows, rows)
    mine = lax.dynamic_slice_in_dim(left, here * rows, rows)
    out = column_block(theirs, scale_all, piece).astype(jnp.bfloat16)
    got = lax.ppermute(out, "tp", [(0, 1), (1, 0)])
    return column_block(mine, scale_all, piece) + got.astype(jnp.float32)


def both_halves(sizes, values):
    if sizes["tp"] != 2:
        return lax.all_gather(values, "tp", axis=0, tiled=True)
    got = lax.ppermute(values, "tp", [(0, 1), (1, 0)])
    first = lax.axis_index("tp") == 0
    return jnp.concatenate([jnp.where(first, values, got), jnp.where(first, got, values)])


def local(
    sizes,
    tokens,
    mix_gain,
    out_gate_w,
    in_gate_w,
    value_w,
    out_gate_scale,
    in_gate_scale,
    value_scale,
    mix_taps,
    conv_gain,
    out_proj_w,
    proj_scale,
    ffn_gain,
    gate_w,
    up_w,
    gate_scale,
    up_scale,
    gate_taps,
    up_taps,
    gate_bias,
    up_bias,
    down_w,
    down_scale,
):
    resid = tokens[0].astype(jnp.float32)
    normed_in = norm_rows(resid, mix_gain).astype(jnp.bfloat16)
    all_rows = lax.all_gather(normed_in, "tp", axis=0, tiled=True)
    vectors = [out_gate_scale, in_gate_scale, value_scale, gate_scale, up_scale, proj_scale, down_scale]
    flat = jnp.concatenate(vectors)
    lines = 24 * (-(-flat.shape[0] // (24 * 128)))
    flat = jnp.pad(flat, (0, lines * 128 - flat.shape[0])).reshape(lines, 128)
    half = jnp.bfloat16
    mix_w = jnp.concatenate([out_gate_w.astype(half), in_gate_w.astype(half), value_w.astype(half)], axis=1)
    flats, mix_all, gate_all, up_all, proj_all = gather_all(
        sizes,
        [flat, mix_w, gate_w.astype(half), up_w.astype(half), out_proj_w.astype(half)],
        [8, 16, 16, 16, 16],
    )
    down_cols = lax.all_gather(down_w.astype(half), "fs", axis=1, tiled=True)
    fs = sizes["fs"]
    flats = flats.reshape(fs, -1)
    scales, at = [], 0
    for vector in vectors:
        scales.append(flats[:, at : at + vector.shape[0]].reshape(-1))
        at += vector.shape[0]
    whole_outgate, whole_ingate, whole_value, whole_gate, whole_up, whole_proj, whole_down = scales
    mix_full = mix_all.reshape(-1, mix_w.shape[1])
    width = out_gate_w.shape[1]
    outgate_rows, ingate_rows, value_rows = (
        mix_full[:, :width],
        mix_full[:, width : 2 * width],
        mix_full[:, 2 * width :],
    )
    proj_cols = proj_all.transpose(1, 0, 2).reshape(proj_all.shape[1], -1)
    out_gate = (
        jnp.dot(all_rows, outgate_rows, preferred_element_type=jnp.float32) * whole_outgate
    ).astype(jnp.bfloat16)
    in_gate = (
        jnp.dot(all_rows, ingate_rows, preferred_element_type=jnp.float32) * whole_ingate
    ).astype(jnp.bfloat16)
    value_in = (
        jnp.dot(all_rows, value_rows, preferred_element_type=jnp.float32) * whole_value
    ).astype(jnp.bfloat16)
    mixed_in = in_gate.astype(jnp.float32) * value_in.astype(jnp.float32)
    conv_out = (out_gate.astype(jnp.float32) * causal_taps(mixed_in, mix_taps)).astype(jnp.bfloat16)
    conv_float = conv_out.astype(jnp.float32)
    channels = conv_float.shape[1] * lax.axis_size("tp")
    sumsq = lax.psum(jnp.sum(conv_float * conv_float, axis=1), "tp")
    mixed = (conv_float * lax.rsqrt(sumsq / channels + epsilon)[:, None] * conv_gain).astype(
        jnp.bfloat16
    )
    summed = summed_half(sizes, mixed, whole_proj, proj_cols)
    first = (resid + summed).astype(jnp.bfloat16)
    resid_two = first.astype(jnp.float32)
    normed_ffn = norm_rows(resid_two, ffn_gain).astype(jnp.bfloat16)
    ffn_all = both_halves(sizes, normed_ffn)
    gate_full = gate_all.reshape(-1, gate_w.shape[1])
    up_full = up_all.reshape(-1, up_w.shape[1])
    gate_sum = jnp.dot(ffn_all, gate_full, preferred_element_type=jnp.float32)
    up_sum = jnp.dot(ffn_all, up_full, preferred_element_type=jnp.float32)
    gate_pre = (gate_sum * whole_gate).astype(jnp.bfloat16)
    up_pre = (up_sum * whole_up).astype(jnp.bfloat16)
    gate_act = causal_taps(gate_pre.astype(jnp.float32), gate_taps) + gate_bias
    up_act = causal_taps(up_pre.astype(jnp.float32), up_taps) + up_bias
    hidden = (jax.nn.silu(gate_act) * up_act).astype(jnp.bfloat16)
    summed_two = summed_half(sizes, hidden, whole_down, down_cols)
    return (resid_two + summed_two).astype(jnp.bfloat16)[None]


def solution(mesh):
    placed = (
        P(("rep", "fs"), "tp", None),
        P(),
        P("fs", "tp"),
        P("fs", "tp"),
        P("fs", "tp"),
        P(("tp", "fs")),
        P(("tp", "fs")),
        P(("tp", "fs")),
        P(None, "tp"),
        P("tp"),
        P("tp", "fs"),
        P("fs"),
        P(),
        P("fs", "tp"),
        P("fs", "tp"),
        P(("tp", "fs")),
        P(("tp", "fs")),
        P(None, "tp"),
        P(None, "tp"),
        P("tp"),
        P("tp"),
        P("tp", "fs"),
        P("fs"),
    )
    return jax.shard_map(
        functools.partial(local, dict(mesh.shape)), mesh=mesh, in_specs=placed, out_specs=P(("rep", "fs"), "tp", None), check_vma=False
    )
```
